768 devices in a mesh: ep: 24 (over z, core), tp: 32 (over y, x).
Axes of the slice: x: 4, y: 8, z: 12, core: 2. Of those that a mesh axis runs over, the one named last changes fastest.
Arguments:
- tokens: bfloat16 [768, 2560], P('ep'), may hold values from -6 to 6
- norm_gain: float32 [2560], replicated, may hold values from 0.1 to 1.9
- route: int32 [768, 4], P('ep'), may hold values from 0 to 23, all different within a row; in each aligned block of 32 rows (0 to 31, 32 to 63, ...) at most 8 rows name the same one
- route_weight: float32 [768, 4], P('ep'), may hold values from 0.1 to 1
- gate_weight: bfloat16 [24, 8960, 2560], P('ep', 'tp'), may hold values from -0.125 to 0.125
- up_weight: bfloat16 [24, 8960, 2560], P('ep', 'tp'), may hold values from -0.125 to 0.125
- down_weight: bfloat16 [24, 8960, 2560], P('ep', 'tp'), may hold values from -0.0625 to 0.0625
Outputs:
- mixed: bfloat16 [768, 2560], P('ep', 'tp')
The draws below stay inside these ranges and needn't reach their ends.
Inputs may be any that keep to these rules, and one draw needn't show every extreme that they name: `route`: each row names 4 different experts. Among the rows of one index of ep no expert is named more than 8 times, a bound that some block reaches.
All inputs are finite; a program needn't handle non-finite values.
Results may differ from the reference program's by a relative error of at most 0.018.
Values may be sent and summed in bfloat16 or wider, within the bound.
No kernel may reach another device: no remote copies, remote signals or barrier semaphores. Data moves between devices by JAX's collectives and lax.ppermute only.
A program may use at most 64 MiB of HBM per device.

```python
import math
import jax
import jax.numpy as jnp
import numpy as np
from jax import lax

D = 2560
FF = 8960
TOP_K = 4
TOK_DEV = 32
EXPERTS = 24
TOKENS = 768
CAP = 8
N_EP = 24
N_TP = 32


def block_levels(own_key, dims, shards, least, top_value):
    loudness = 1.0
    for axis_at, blocks in shards:
        steps = jax.random.uniform(jax.random.fold_in(jax.random.fold_in(own_key, 6), axis_at), (blocks,), jnp.float32, least / len(shards), top_value / len(shards))
        loudness = loudness * jnp.repeat(jnp.exp(steps), dims[axis_at] // blocks).reshape((-1,) + (1,) * (len(dims) - 1 - axis_at))
    return loudness


def shared_out(own_key, own, number, rows, number_of, top, limit, lean):
    ranking = jax.random.permutation(own_key, number_of)
    packed, common = shares(number_of, rows * top, limit, lean, True), shares(number_of, rows * top, limit, lean, False)
    places = jnp.arange(number_of)

    def named(tallies, rotation):
        used = int((tallies > 0).sum())
        fixed = max(1, used // 4)
        shifted = fixed + (places - fixed + rotation * (used - fixed)) % max(1, number_of - fixed)
        return jnp.zeros((number_of,), jnp.int32).at[ranking[jnp.where(places < fixed, places, shifted)]].set(jnp.asarray(tallies, jnp.int32))

    tallies = jnp.where(number % 4 == 0, named(packed, number // 4), named(common, number - number // 4 - 1))
    mixed = jax.random.permutation(jax.random.fold_in(own, 3), number_of)
    donor, taker = mixed[0:number_of // 2 * 2:2], mixed[1:number_of // 2 * 2:2]
    room = jnp.minimum(tallies[donor] - 1, limit - tallies[taker]) // 2
    room = jnp.where((donor == ranking[0]) | (taker == ranking[0]) | (tallies[taker] == 0), 0, jnp.maximum(room, 0))
    shifted = jax.random.randint(jax.random.fold_in(own, 4), (number_of // 2,), 0, 1 << 20) % (room + 1)
    tallies = tallies.at[donor].add(-shifted).at[taker].add(shifted)
    labels = jnp.searchsorted(jnp.cumsum(tallies), jnp.arange(rows * top), side="right").astype(jnp.int32)
    listing = labels.reshape(top, rows).T
    listing = listing[jax.random.permutation(jax.random.fold_in(own, 1), rows)]
    rotation = jax.random.randint(jax.random.fold_in(own, 2), (rows, 1), 0, top)
    return jnp.take_along_axis(listing, (jnp.arange(top)[None, :] + rotation) % top, axis=1)


def shares(number_of, total, most, slope, full):
    loads = [(1 << 20) // math.isqrt(standing ** slope) + 1 for standing in range(1, number_of + 1)]
    largest = most if full else min(most, max(-(-total // number_of), total * loads[0] // sum(loads)))
    least = 1 if total - largest >= number_of - 1 else 0
    counts, rest = [largest] + [least] * (number_of - 1), total - largest - least * (number_of - 1)
    while rest > 0:
        movable = [i for i in range(1, number_of) if counts[i] < largest] or [i for i in range(1, number_of) if counts[i] < most]
        whole, remaining = sum([loads[i] for i in movable]), rest
        for i in movable:
            addition = min(most - counts[i], max(1, remaining * loads[i] // whole), rest)
            counts[i] = counts[i] + addition
            rest = rest - addition
    return np.array(counts)


def normal_values(stream_key, dims, spread, bound, cuts=(), kind=jnp.bfloat16):
    entries = jax.random.normal(stream_key, dims, jnp.float32) * spread
    if len(cuts) > 0:
        entries = block_levels(stream_key, dims, cuts, -0.22, 0.18) * entries
    return jnp.clip(entries, min=-bound, max=bound).astype(kind)


def setup_inputs(seed: int = 0) -> dict:
    streams_of = jax.random.split(jax.random.key(seed), 8)
    tokens = normal_values(streams_of[0], (TOKENS, D), 1.0, 6.0, ((0, 24),))
    norm_gain = jnp.clip(1.0 + 0.18 * jax.random.normal(streams_of[1], (D,), jnp.float32), 0.1, 1.9)
    route_keys = jax.random.split(jax.random.fold_in(streams_of[2], 1), TOKENS // TOK_DEV)
    route_turns = jax.random.permutation(jax.random.fold_in(streams_of[2], 3), TOKENS // TOK_DEV)
    route = jax.vmap(lambda own, number: shared_out(jax.random.fold_in(streams_of[2], 2), own, number, TOK_DEV, EXPERTS, TOP_K, CAP, 2))(route_keys, route_turns).reshape((TOKENS, TOP_K))
    route_weight = jnp.clip(0.1 + 0.9 * jax.random.uniform(streams_of[3], (TOKENS, TOP_K), jnp.float32) ** block_levels(streams_of[3], (TOKENS, TOP_K), ((0, 24),), -0.2, 0.2), 0.1, 1.0)
    gate_weight = normal_values(streams_of[4], (EXPERTS, FF, D), D ** -0.5, 0.125, ((0, 24), (1, 32)))
    up_weight = normal_values(streams_of[5], (EXPERTS, FF, D), D ** -0.5, 0.125, ((0, 24), (1, 32)))
    down_weight = normal_values(streams_of[6], (EXPERTS, FF, D), FF ** -0.5, 0.0625, ((0, 24), (1, 32)))
    return {"tokens": tokens, "norm_gain": norm_gain, "route": route, "route_weight": route_weight, "gate_weight": gate_weight, "up_weight": up_weight, "down_weight": down_weight}


epsilon = 1e-06

def reference(tokens, norm_gain, route, route_weight, gate_weight, up_weight, down_weight):
    values = tokens.astype(jnp.float32)
    scaled = values * lax.rsqrt(lax.optimization_barrier(jnp.mean(values * values, axis=-1, keepdims=True)) + epsilon)
    normed = (scaled * norm_gain).astype(jnp.bfloat16)
    flat_route = route.reshape(N_EP, TOK_DEV * TOP_K)
    onehot = (flat_route[:, :, None] == jnp.arange(EXPERTS, dtype=jnp.int32)[None, None, :]).astype(jnp.int32)
    slot_number = lax.optimization_barrier(jnp.sum((jnp.cumsum(onehot, axis=1) - 1) * onehot, axis=-1)).astype(jnp.int32)
    source = jnp.arange(N_EP, dtype=jnp.int32)[:, None]
    slot_index = ((flat_route * N_EP + source) * CAP + slot_number).reshape(TOKENS * TOP_K).astype(jnp.int32)
    repeated = jnp.repeat(normed, TOP_K, axis=0)
    buffer = jnp.zeros((EXPERTS * N_EP * CAP, D), jnp.bfloat16).at[slot_index].set(repeated)
    buffer = buffer.reshape(EXPERTS, N_EP * CAP, D)

    def expert(operands):
        inputs, w_gate, w_up, w_down = operands
        gate = jnp.dot(inputs, w_gate.T, preferred_element_type=jnp.float32)
        upward = jnp.dot(inputs, w_up.T, preferred_element_type=jnp.float32)
        hidden = (jax.nn.silu(gate) * upward).astype(jnp.bfloat16)
        hidden_blocks = hidden.reshape(N_EP * CAP, N_TP, FF // N_TP).astype(jnp.float32)
        down_blocks = w_down.reshape(N_TP, FF // N_TP, D).astype(jnp.float32)
        block_sum = jnp.einsum('rbf,bfd->brd', hidden_blocks, down_blocks).astype(jnp.bfloat16)
        block_sum = lax.optimization_barrier(block_sum)
        return lax.optimization_barrier(jnp.sum(block_sum.astype(jnp.float32), axis=0)).astype(jnp.bfloat16)
    results = lax.map(expert, (buffer, gate_weight, up_weight, down_weight)).reshape(EXPERTS * N_EP * CAP, D)
    picked = results[slot_index].reshape(TOKENS, TOP_K, D).astype(jnp.float32)
    mixed = lax.optimization_barrier(jnp.sum(route_weight[:, :, None] * picked, axis=1))
    return mixed.astype(jnp.bfloat16)
```

```python
import jax
import jax.numpy as jnp
from jax import lax
from jax.experimental import pallas as pl
from jax.experimental.pallas import tpu as pltpu
from jax.sharding import Mesh
from jax.sharding import PartitionSpec as P

epsilon = 1e-06
bf16 = jnp.bfloat16
f32 = jnp.float32

Z, C, Y, X = 12, 2, 8, 4
EP = Z * C
TP = Y * X


def whole_vmem(count):
    return [pl.BlockSpec(memory_space=pltpu.VMEM)] * count


def slots_of(route_t, experts, rows):
    expert = lax.broadcasted_iota(jnp.int32, (experts, rows), 0)
    named = jnp.zeros((experts, rows), f32)
    for k in range(route_t.shape[0]):
        named = named + (route_t[k : k + 1, :] == expert).astype(f32)
    before = lax.broadcasted_iota(jnp.int32, (rows, rows), 0) < lax.broadcasted_iota(
        jnp.int32, (rows, rows), 1
    )
    earlier = jnp.dot(named, before.astype(f32), preferred_element_type=f32)
    return named, earlier


def place_kernel(at_ref, tokens_ref, gain_ref, route_ref, send_ref):
    rows, width = tokens_ref.shape
    experts, cap, share = EP, send_ref.shape[0] // EP, send_ref.shape[1]
    values = tokens_ref[...].astype(f32)
    scale = lax.rsqrt(jnp.mean(values * values, axis=-1, keepdims=True) + epsilon)
    start = pl.multiple_of(at_ref[0] * share, 128)
    own = tokens_ref[:, pl.ds(start, share)].astype(f32)
    normed = (own * scale * gain_ref[:, pl.ds(start, share)]).astype(bf16)
    named, earlier = slots_of(route_ref[...], experts, rows)
    spots = experts * cap
    spot = lax.broadcasted_iota(jnp.int32, (spots, experts), 0)
    spread = (spot // cap == lax.broadcasted_iota(jnp.int32, (spots, experts), 1)).astype(f32)
    hit = jnp.dot(spread, named, preferred_element_type=f32)
    count = jnp.dot(spread, earlier, preferred_element_type=f32)
    slot = (lax.broadcasted_iota(jnp.int32, (spots, rows), 0) % cap).astype(f32)
    placing = jnp.where(count == slot, hit, 0.0).astype(bf16)
    send_ref[...] = jnp.dot(placing, normed, preferred_element_type=f32).astype(bf16)


def expert_kernel(rows_ref, gate_ref, up_ref, down_ref, out_ref):
    parts, _, share = rows_ref.shape
    contract = (((1,), (1,)), ((), ()))
    gate = up = None
    for p in range(parts):
        rows = rows_ref[p]
        cols = slice(p * share, (p + 1) * share)
        g = lax.dot_general(rows, gate_ref[:, cols], contract, preferred_element_type=f32)
        u = lax.dot_general(rows, up_ref[:, cols], contract, preferred_element_type=f32)
        gate = g if gate is None else gate + g
        up = u if up is None else up + u
    hidden = (gate / (1.0 + jnp.exp(-gate)) * up).astype(bf16)
    block = share // Y
    sums = jnp.dot(hidden, down_ref[...], preferred_element_type=f32).astype(bf16)
    for p in range(parts):
        blocks = [sums[:, (y * X + p) * block : (y * X + p + 1) * block] for y in range(Y)]
        out_ref[p] = jnp.concatenate(blocks, axis=1)


def sum_x_kernel(in_ref, out_ref):
    total = in_ref[0].astype(f32)
    for p in range(1, in_ref.shape[0]):
        total = total + in_ref[p].astype(f32)
    total = total.astype(bf16)
    share = out_ref.shape[2]
    for p in range(out_ref.shape[0]):
        out_ref[p] = total[:, p * share : (p + 1) * share]


def sum_y_kernel(in_ref, out_ref):
    total = in_ref[0].astype(f32)
    for p in range(1, in_ref.shape[0]):
        total = total + in_ref[p].astype(f32)
    out_ref[...] = total.astype(bf16)


def mix_kernel(got_ref, route_ref, weight_ref, out_ref):
    rows = out_ref.shape[0]
    spots = got_ref.shape[0]
    experts, cap = EP, spots // EP
    route_t = route_ref[...]
    named, earlier = slots_of(route_t, experts, rows)
    expert = lax.broadcasted_iota(jnp.int32, (experts, rows), 0)
    weight = jnp.zeros((experts, rows), f32)
    for k in range(route_t.shape[0]):
        weight = weight + jnp.where(route_t[k : k + 1, :] == expert, weight_ref[k : k + 1, :], 0.0)
    spot = lax.broadcasted_iota(jnp.int32, (spots, experts), 0)
    spread = (spot // cap == lax.broadcasted_iota(jnp.int32, (spots, experts), 1)).astype(f32)
    exact = lax.Precision.HIGHEST
    count = jnp.dot(spread, earlier, preferred_element_type=f32)
    hit = jnp.dot(spread, weight, preferred_element_type=f32, precision=exact)
    slot = (lax.broadcasted_iota(jnp.int32, (spots, rows), 0) % cap).astype(f32)
    chosen = jnp.where(count == slot, hit, 0.0)
    mixed = lax.dot_general(
        chosen,
        got_ref[...].astype(f32),
        (((0,), (0,)), ((), ())),
        preferred_element_type=f32,
        precision=exact,
    )
    out_ref[...] = mixed.astype(bf16)


def on_device(tokens, norm_gain, route, route_weight, gate_weight, up_weight, down_weight):
    tok_rows, width = tokens.shape
    cap = 8
    quarter = width // X
    share = width // TP
    spots = EP * cap
    route_t = route.T
    weight_t = route_weight.T
    at = lax.axis_index("x").astype(jnp.int32).reshape(1)

    send = pl.pallas_call(
        place_kernel,
        in_specs=[pl.BlockSpec(memory_space=pltpu.SMEM)] + whole_vmem(3),
        out_specs=pl.BlockSpec(memory_space=pltpu.VMEM),
        out_shape=jax.ShapeDtypeStruct((spots, quarter), bf16),
        name="place",
    )(at, tokens, norm_gain.reshape(1, width), route_t)
    arrived = lax.all_to_all(send.reshape(EP, cap, quarter), ("z", "c"), 0, 0, tiled=True)
    rows = lax.all_gather(arrived.reshape(spots, quarter), "x", axis=0, tiled=False)
    part = pl.pallas_call(
        expert_kernel,
        in_specs=whole_vmem(4),
        out_specs=pl.BlockSpec(memory_space=pltpu.VMEM),
        out_shape=jax.ShapeDtypeStruct((X, spots, quarter), bf16),
        name="expert",
    )(rows, gate_weight[0], up_weight[0], down_weight[0])
    part = lax.all_to_all(part, "x", 0, 0, tiled=True)
    part = pl.pallas_call(
        sum_x_kernel,
        in_specs=whole_vmem(1),
        out_specs=pl.BlockSpec(memory_space=pltpu.VMEM),
        out_shape=jax.ShapeDtypeStruct((Y, spots, share), bf16),
        name="sum_x",
    )(part)
    part = lax.all_to_all(part, "y", 0, 0, tiled=True)
    done = pl.pallas_call(
        sum_y_kernel,
        in_specs=whole_vmem(1),
        out_specs=pl.BlockSpec(memory_space=pltpu.VMEM),
        out_shape=jax.ShapeDtypeStruct((spots, share), bf16),
        name="sum_y",
    )(part)
    back = lax.all_to_all(done.reshape(EP, cap, share), ("z", "c"), 0, 0, tiled=True)
    return pl.pallas_call(
        mix_kernel,
        in_specs=whole_vmem(3),
        out_specs=pl.BlockSpec(memory_space=pltpu.VMEM),
        out_shape=jax.ShapeDtypeStruct((tok_rows, share), bf16),
        name="mix",
    )(back.reshape(spots, share), route_t, weight_t)


def solution(mesh):
    fine = Mesh(mesh.devices.reshape(Z, C, Y, X), ("z", "c", "y", "x"))
    ep, tp = ("z", "c"), ("y", "x")
    placed = (
        P(ep, None),
        P(),
        P(ep, None),
        P(ep, None),
        P(ep, tp, None),
        P(ep, tp, None),
        P(ep, tp, None),
    )
    return jax.shard_map(
        on_device, mesh=fine, in_specs=placed, out_specs=P(ep, tp), check_vma=False
    )
```

```python
import jax
import jax.numpy as jnp
from jax import lax
from jax.experimental import pallas as pl
from jax.experimental.pallas import tpu as pltpu
from jax.sharding import Mesh
from jax.sharding import PartitionSpec as P

epsilon = 1e-06
bf16 = jnp.bfloat16
f32 = jnp.float32

Z, C, Y, X = 12, 2, 8, 4
EP = Z * C
TP = Y * X
CAP = 8
LANES = 128
SCOPED = 16 << 20
VMEM = pl.BlockSpec(memory_space=pltpu.VMEM)


HBM = pl.BlockSpec(memory_space=pl.ANY)


def near(array):
    return pltpu.with_memory_space_constraint(array, pltpu.VMEM)


def far(array):
    return pltpu.with_memory_space_constraint(array, pltpu.HBM)


def local(kernel, name, specs, outs, scratch=()):
    return pl.pallas_call(
        kernel,
        in_specs=specs,
        out_specs=tuple(VMEM for _ in outs) if isinstance(outs, tuple) else VMEM,
        out_shape=outs,
        scratch_shapes=scratch,
        compiler_params=pltpu.CompilerParams(vmem_limit_bytes=SCOPED),
        name=name,
    )


def summed(ref):
    total = ref[0].astype(f32)
    for p in range(1, ref.shape[0]):
        total = total + ref[p].astype(f32)
    return total


def per_slot(table):
    rows = table.shape[1]
    lines = [jnp.broadcast_to(table[e : e + 1, :], (CAP, rows)) for e in range(table.shape[0])]
    return jnp.concatenate(lines, axis=0)


def place_kernel(at_ref, *refs):
    sources, (send_ref, chosen_ref) = refs[:4], refs[4:6]
    (tokens_ref, gain_ref, route_ref, weight_ref), sems = refs[6:10], refs[10]
    copies = [
        pltpu.make_async_copy(source, there, sems.at[i])
        for i, (source, there) in enumerate(zip(sources, refs[6:10]))
    ]
    for copy in copies:
        copy.start()
    for copy in copies:
        copy.wait()
    rows = tokens_ref.shape[0]
    share = send_ref.shape[1]
    values = tokens_ref[...].astype(f32)
    scale = lax.rsqrt(jnp.mean(values * values, axis=-1, keepdims=True) + epsilon)
    start = pl.multiple_of(at_ref[0] * share, LANES)
    own = tokens_ref[:, pl.ds(start, share)].astype(f32)
    gain = gain_ref[pl.ds(start, share)].reshape(1, share)
    normed = (own * scale * gain).astype(bf16)
    expert = lax.broadcasted_iota(jnp.int32, (EP, rows), 0)
    named = jnp.zeros((EP, rows), f32)
    weight = jnp.zeros((EP, rows), f32)
    for k in range(route_ref.shape[0]):
        same = route_ref[k : k + 1, :] == expert
        named = jnp.where(same, 1.0, named)
        weight = jnp.where(same, weight_ref[k : k + 1, :], weight)
    before = lax.broadcasted_iota(jnp.int32, (rows, rows), 0) < lax.broadcasted_iota(
        jnp.int32, (rows, rows), 1
    )
    earlier = jnp.dot(named, before.astype(f32), preferred_element_type=f32)
    taken = per_slot(jnp.where(named > 0.0, earlier, -1.0))
    slot = (lax.broadcasted_iota(jnp.int32, taken.shape, 0) % CAP).astype(f32)
    here = taken == slot
    placing = jnp.where(here, 1.0, 0.0).astype(bf16)
    send_ref[...] = jnp.dot(placing, normed, preferred_element_type=f32).astype(bf16)
    chosen_ref[...] = jnp.where(here, per_slot(weight), 0.0).T


def expert_kernel(rows_ref, gate_ref, up_far, down_far, out_ref, up_ref, down_ref, sems):
    parts, _, share = rows_ref.shape
    spans = [slice(p * share, (p + 1) * share) for p in range(parts)]
    fetches = [
        pltpu.make_async_copy(up_far.at[:, cols], up_ref.at[:, cols], sems.at[p])
        for p, cols in enumerate(spans)
    ] + [
        pltpu.make_async_copy(down_far.at[:, cols], down_ref.at[:, cols], sems.at[parts + p])
        for p, cols in enumerate(spans)
    ]
    for fetch in fetches:
        fetch.start()
    contract = (((1,), (1,)), ((), ()))
    gate = up = None
    for p, cols in enumerate(spans):
        g = lax.dot_general(gate_ref[:, cols], rows_ref[p], contract, preferred_element_type=f32)
        gate = g if gate is None else gate + g
    for p, cols in enumerate(spans):
        fetches[p].wait()
        u = lax.dot_general(up_ref[:, cols], rows_ref[p], contract, preferred_element_type=f32)
        up = u if up is None else up + u
    hidden = (gate / (1.0 + jnp.exp(-gate)) * up).T.astype(bf16)
    block = share // Y
    for p, cols in enumerate(spans):
        fetches[parts + p].wait()
        sums = jnp.dot(hidden, down_ref[:, cols], preferred_element_type=f32).astype(bf16)
        for i in range(Y):
            y, x = divmod(p * Y + i, X)
            out_ref[x, :, y * block : (y + 1) * block] = sums[:, i * block : (i + 1) * block]


def sum_x_kernel(in_ref, out_ref):
    total = summed(in_ref).T
    block = total.shape[0] // Y
    half = block // 2
    for y in range(Y):
        piece = total[y * block : (y + 1) * block]
        out_ref[y, :block] = piece[:, :LANES].astype(bf16)
        tail = piece[:, LANES:]
        out_ref[y, block:] = jnp.concatenate([tail[:half], tail[half:]], axis=1).astype(bf16)


def sum_y_kernel(in_ref, out_ref):
    total = summed(in_ref)
    block = out_ref.shape[1]
    rest = out_ref.shape[0] - LANES
    tail = jnp.concatenate([total[block:, :rest], total[block:, rest:]], axis=0)
    out_ref[:LANES] = total[:block].T.astype(bf16)
    out_ref[LANES:] = tail.T.astype(bf16)


def mix_kernel(got_ref, chosen_ref, out_ref):
    mixed = jnp.dot(
        chosen_ref[...],
        got_ref[...].astype(f32),
        preferred_element_type=f32,
        precision=lax.Precision.HIGHEST,
    )
    out_ref[...] = mixed.astype(bf16)


def on_device(tokens, norm_gain, route, route_weight, gate_weight, up_weight, down_weight):
    tok_rows, width = tokens.shape
    quarter = width // X
    share = width // TP
    spots = EP * CAP
    ep = ("z", "c")
    at = lax.axis_index("x").astype(jnp.int32).reshape(1)

    inputs = (tokens, norm_gain, route.T, route_weight.T)
    send, chosen = local(
        place_kernel,
        "place",
        [pl.BlockSpec(memory_space=pltpu.SMEM)] + [HBM] * 4,
        (pltpu.VMEM((spots, quarter), bf16), pltpu.VMEM((tok_rows, spots), f32)),
        scratch=[pltpu.VMEM(a.shape, a.dtype) for a in inputs]
        + [pltpu.SemaphoreType.DMA((len(inputs),))],
    )(at, *[far(a) for a in inputs])
    arrived = lax.all_to_all(send.reshape(EP, CAP, quarter), ep, 0, 0, tiled=True)
    rows = lax.all_gather(arrived.reshape(spots, quarter), "x", axis=0, tiled=False)
    part = local(
        expert_kernel,
        "expert",
        [VMEM, VMEM, HBM, HBM],
        pltpu.VMEM((X, spots, quarter), bf16),
        scratch=[
            pltpu.VMEM(up_weight.shape[1:], bf16),
            pltpu.VMEM(down_weight.shape[1:], bf16),
            pltpu.SemaphoreType.DMA((2 * X,)),
        ],
    )(near(rows), near(gate_weight[0]), far(up_weight[0]), far(down_weight[0]))
    part = lax.all_to_all(part, "x", 0, 0, tiled=True)
    packed = spots * share // LANES
    part = local(sum_x_kernel, "sum_x", [VMEM], pltpu.VMEM((Y, packed, LANES), bf16))(near(part))
    part = lax.all_to_all(part, "y", 0, 0, tiled=True)
    done = local(sum_y_kernel, "sum_y", [VMEM], pltpu.VMEM((spots, share), bf16))(near(part))
    back = lax.all_to_all(done.reshape(EP, CAP, share), ep, 0, 0, tiled=True)
    mixed = jax.ShapeDtypeStruct((tok_rows, share), bf16)
    return local(mix_kernel, "mix", [VMEM, VMEM], mixed)(
        near(back.reshape(spots, share)), near(chosen)
    )


def solution(mesh):
    fine = Mesh(mesh.devices.reshape(Z, C, Y, X), ("z", "c", "y", "x"))
    ep, tp = ("z", "c"), ("y", "x")
    placed = (
        P(ep, None),
        P(),
        P(ep, None),
        P(ep, None),
        P(ep, tp, None),
        P(ep, tp, None),
        P(ep, tp, None),
    )
    return jax.shard_map(
        on_device, mesh=fine, in_specs=placed, out_specs=P(ep, tp), check_vma=False
    )
```

```python
import jax
import jax.numpy as jnp
from jax import lax
from jax.experimental import pallas as pl
from jax.experimental.pallas import tpu as pltpu
from jax.sharding import Mesh
from jax.sharding import PartitionSpec as P

epsilon = 1e-06
bf16 = jnp.bfloat16
f32 = jnp.float32

Z, C, Y, X = 12, 2, 8, 4
EP = Z * C
TP = Y * X
CAP = 8
LANES = 128
SCOPED = 16 << 20
VMEM = pl.BlockSpec(memory_space=pltpu.VMEM)


HBM = pl.BlockSpec(memory_space=pl.ANY)


def near(array):
    return pltpu.with_memory_space_constraint(array, pltpu.VMEM)


def far(array):
    return pltpu.with_memory_space_constraint(array, pltpu.HBM)


def local(kernel, name, specs, outs, scratch=(), cost=None):
    return pl.pallas_call(
        kernel,
        in_specs=specs,
        out_specs=tuple(VMEM for _ in outs) if isinstance(outs, tuple) else VMEM,
        out_shape=outs,
        scratch_shapes=scratch,
        cost_estimate=cost,
        compiler_params=pltpu.CompilerParams(vmem_limit_bytes=SCOPED),
        name=name,
    )


def summed(ref):
    total = ref[0].astype(f32)
    for p in range(1, ref.shape[0]):
        total = total + ref[p].astype(f32)
    return total


def per_slot(table):
    rows = table.shape[1]
    lines = [jnp.broadcast_to(table[e : e + 1, :], (CAP, rows)) for e in range(table.shape[0])]
    return jnp.concatenate(lines, axis=0)


def place_kernel(*refs):
    sources, (send_ref, chosen_ref) = refs[:4], refs[4:6]
    (tokens_ref, gain_ref, route_ref, weight_ref), sems = refs[6:10], refs[10]
    copies = [
        pltpu.make_async_copy(source, there, sems.at[i])
        for i, (source, there) in enumerate(zip(sources, refs[6:10]))
    ]
    for copy in copies:
        copy.start()
    for copy in copies:
        copy.wait()
    rows = tokens_ref.shape[0]
    share = send_ref.shape[1]
    values = tokens_ref[...].astype(f32)
    scale = lax.rsqrt(jnp.mean(values * values, axis=-1, keepdims=True) + epsilon)
    start = pl.multiple_of(lax.axis_index("x") * share, LANES)
    own = tokens_ref[:, pl.ds(start, share)].astype(f32)
    gain = gain_ref[pl.ds(start, share)].reshape(1, share)
    normed = (own * scale * gain).astype(bf16)
    expert = lax.broadcasted_iota(jnp.int32, (EP, rows), 0)
    named = jnp.zeros((EP, rows), f32)
    weight = jnp.zeros((EP, rows), f32)
    for k in range(route_ref.shape[0]):
        same = route_ref[k : k + 1, :] == expert
        named = jnp.where(same, 1.0, named)
        weight = jnp.where(same, weight_ref[k : k + 1, :], weight)
    before = lax.broadcasted_iota(jnp.int32, (rows, rows), 0) < lax.broadcasted_iota(
        jnp.int32, (rows, rows), 1
    )
    earlier = jnp.dot(named, before.astype(f32), preferred_element_type=f32)
    taken = per_slot(jnp.where(named > 0.0, earlier, -1.0))
    slot = (lax.broadcasted_iota(jnp.int32, taken.shape, 0) % CAP).astype(f32)
    here = taken == slot
    placing = jnp.where(here, 1.0, 0.0).astype(bf16)
    send_ref[...] = jnp.dot(placing, normed, preferred_element_type=f32).astype(bf16)
    chosen_ref[...] = jnp.where(here, per_slot(weight), 0.0).T


def expert_kernel(rows_ref, gate_ref, up_ref, down_ref, out_ref):
    parts, _, share = rows_ref.shape
    spans = [slice(p * share, (p + 1) * share) for p in range(parts)]
    contract = (((1,), (1,)), ((), ()))
    gate = up = None
    for p, cols in enumerate(spans):
        g = lax.dot_general(gate_ref[:, cols], rows_ref[p], contract, preferred_element_type=f32)
        gate = g if gate is None else gate + g
    for p, cols in enumerate(spans):
        u = lax.dot_general(up_ref[:, cols], rows_ref[p], contract, preferred_element_type=f32)
        up = u if up is None else up + u
    hidden = (gate / (1.0 + jnp.exp(-gate)) * up).T.astype(bf16)
    block = share // Y
    for p, cols in enumerate(spans):
        sums = jnp.dot(hidden, down_ref[:, cols], preferred_element_type=f32).astype(bf16)
        for i in range(Y):
            y, x = divmod(p * Y + i, X)
            out_ref[x, :, y * block : (y + 1) * block] = sums[:, i * block : (i + 1) * block]


def sum_x_kernel(in_ref, out_ref):
    total = summed(in_ref).T
    block = total.shape[0] // Y
    half = block // 2
    for y in range(Y):
        piece = total[y * block : (y + 1) * block]
        out_ref[y, :block] = piece[:, :LANES].astype(bf16)
        tail = piece[:, LANES:]
        out_ref[y, block:] = jnp.concatenate([tail[:half], tail[half:]], axis=1).astype(bf16)


def sum_y_kernel(in_ref, out_ref):
    total = summed(in_ref)
    block = out_ref.shape[1]
    rest = out_ref.shape[0] - LANES
    tail = jnp.concatenate([total[block:, :rest], total[block:, rest:]], axis=0)
    out_ref[:LANES] = total[:block].T.astype(bf16)
    out_ref[LANES:] = tail.T.astype(bf16)


def mix_kernel(got_ref, chosen_ref, out_ref):
    mixed = jnp.dot(
        chosen_ref[...],
        got_ref[...].astype(f32),
        preferred_element_type=f32,
        precision=lax.Precision.HIGHEST,
    )
    out_ref[...] = mixed.astype(bf16)


def on_device(tokens, norm_gain, route, route_weight, gate_weight, up_weight, down_weight):
    tok_rows, width = tokens.shape
    quarter = width // X
    share = width // TP
    spots = EP * CAP
    ep = ("z", "c")
    inputs = (tokens, norm_gain, route.T, route_weight.T)
    send, chosen = local(
        place_kernel,
        "place",
        [HBM] * 4,
        (pltpu.VMEM((spots, quarter), bf16), pltpu.VMEM((tok_rows, spots), f32)),
        scratch=[pltpu.VMEM(a.shape, a.dtype) for a in inputs]
        + [pltpu.SemaphoreType.DMA((len(inputs),))],
        cost=pl.CostEstimate(flops=10**10, transcendentals=0, bytes_accessed=10**6),
    )(*[far(a) for a in inputs])
    arrived = lax.all_to_all(send.reshape(EP, CAP, quarter), ep, 0, 0, tiled=True)
    rows = lax.all_gather(arrived.reshape(spots, quarter), "x", axis=0, tiled=False)
    part = local(
        expert_kernel,
        "expert",
        [VMEM] * 4,
        pltpu.VMEM((X, spots, quarter), bf16),
    )(near(rows), near(gate_weight[0]), near(up_weight[0]), near(down_weight[0]))
    part = lax.all_to_all(part, "x", 0, 0, tiled=True)
    packed = spots * share // LANES
    part = local(sum_x_kernel, "sum_x", [VMEM], pltpu.VMEM((Y, packed, LANES), bf16))(near(part))
    part = lax.all_to_all(part, "y", 0, 0, tiled=True)
    done = local(sum_y_kernel, "sum_y", [VMEM], pltpu.VMEM((spots, share), bf16))(near(part))
    back = lax.all_to_all(done.reshape(EP, CAP, share), ep, 0, 0, tiled=True)
    mixed = jax.ShapeDtypeStruct((tok_rows, share), bf16)
    return local(mix_kernel, "mix", [VMEM, VMEM], mixed)(
        near(back.reshape(spots, share)), near(chosen)
    )


def solution(mesh):
    fine = Mesh(mesh.devices.reshape(Z, C, Y, X), ("z", "c", "y", "x"))
    ep, tp = ("z", "c"), ("y", "x")
    placed = (
        P(ep, None),
        P(),
        P(ep, None),
        P(ep, None),
        P(ep, tp, None),
        P(ep, tp, None),
        P(ep, tp, None),
    )
    return jax.shard_map(
        on_device, mesh=fine, in_specs=placed, out_specs=P(ep, tp), check_vma=False
    )
```

```python
import jax
import jax.numpy as jnp
from jax import lax
from jax.experimental import pallas as pl
from jax.experimental.pallas import tpu as pltpu
from jax.sharding import Mesh
from jax.sharding import PartitionSpec as P

epsilon = 1e-06
bf16 = jnp.bfloat16
f32 = jnp.float32

Z, C, Y, X = 12, 2, 8, 4
EP = Z * C
TP = Y * X
CAP = 8
LANES = 128
SCOPED = 16 << 20
VMEM = pl.BlockSpec(memory_space=pltpu.VMEM)


HBM = pl.BlockSpec(memory_space=pl.ANY)


def near(array):
    return pltpu.with_memory_space_constraint(array, pltpu.VMEM)


def far(array):
    return pltpu.with_memory_space_constraint(array, pltpu.HBM)


def local(kernel, name, specs, outs, scratch=(), cost=None):
    return pl.pallas_call(
        kernel,
        in_specs=specs,
        out_specs=tuple(VMEM for _ in outs) if isinstance(outs, tuple) else VMEM,
        out_shape=outs,
        scratch_shapes=scratch,
        cost_estimate=cost,
        compiler_params=pltpu.CompilerParams(vmem_limit_bytes=SCOPED),
        name=name,
    )


def summed(ref):
    total = ref[0].astype(f32)
    for p in range(1, ref.shape[0]):
        total = total + ref[p].astype(f32)
    return total


def per_slot(table):
    rows = table.shape[1]
    lines = [jnp.broadcast_to(table[e : e + 1, :], (CAP, rows)) for e in range(table.shape[0])]
    return jnp.concatenate(lines, axis=0)


def place_kernel(*refs):
    sources, (send_ref, chosen_ref) = refs[:4], refs[4:6]
    (tokens_ref, gain_ref, route_ref, weight_ref), sems = refs[6:10], refs[10]
    copies = [
        pltpu.make_async_copy(source, there, sems.at[i])
        for i, (source, there) in enumerate(zip(sources, refs[6:10]))
    ]
    for i in (2, 3, 0, 1):
        copies[i].start()
    rows = tokens_ref.shape[0]
    share = send_ref.shape[1]
    before = lax.broadcasted_iota(jnp.int32, (rows, rows), 0) < lax.broadcasted_iota(
        jnp.int32, (rows, rows), 1
    )
    expert = lax.broadcasted_iota(jnp.int32, (EP, rows), 0)
    copies[2].wait()
    copies[3].wait()
    named = jnp.zeros((EP, rows), f32)
    weight = jnp.zeros((EP, rows), f32)
    for k in range(route_ref.shape[0]):
        same = route_ref[k : k + 1, :] == expert
        named = jnp.where(same, 1.0, named)
        weight = jnp.where(same, weight_ref[k : k + 1, :], weight)
    earlier = jnp.dot(named, before.astype(f32), preferred_element_type=f32)
    taken = per_slot(jnp.where(named > 0.0, earlier, -1.0))
    slot = (lax.broadcasted_iota(jnp.int32, taken.shape, 0) % CAP).astype(f32)
    here = taken == slot
    placing = jnp.where(here, 1.0, 0.0).astype(bf16)
    chosen_ref[...] = jnp.where(here, per_slot(weight), 0.0).T
    copies[0].wait()
    copies[1].wait()
    values = tokens_ref[...].astype(f32)
    scale = lax.rsqrt(jnp.mean(values * values, axis=-1, keepdims=True) + epsilon)
    start = pl.multiple_of(lax.axis_index("x") * share, LANES)
    own = tokens_ref[:, pl.ds(start, share)].astype(f32)
    gain = gain_ref[pl.ds(start, share)].reshape(1, share)
    normed = (own * scale * gain).astype(bf16)
    send_ref[...] = jnp.dot(placing, normed, preferred_element_type=f32).astype(bf16)


def expert_kernel(rows_ref, gate_ref, up_ref, down_ref, out_ref):
    parts, _, share = rows_ref.shape
    spans = [slice(p * share, (p + 1) * share) for p in range(parts)]
    contract = (((1,), (1,)), ((), ()))
    gate = up = None
    for p, cols in enumerate(spans):
        g = lax.dot_general(gate_ref[:, cols], rows_ref[p], contract, preferred_element_type=f32)
        gate = g if gate is None else gate + g
    for p, cols in enumerate(spans):
        u = lax.dot_general(up_ref[:, cols], rows_ref[p], contract, preferred_element_type=f32)
        up = u if up is None else up + u
    hidden = (gate / (1.0 + jnp.exp(-gate)) * up).astype(bf16).T
    block = share // Y
    for p, cols in enumerate(spans):
        sums = jnp.dot(hidden, down_ref[:, cols], preferred_element_type=f32).astype(bf16).T
        for i in range(Y):
            packed(sums[i * block : (i + 1) * block], out_ref.at[i], p)


def packed(piece, out, at):
    block = piece.shape[0]
    tail = piece[:, LANES:]
    out[at, :block] = piece[:, :LANES].astype(bf16)
    out[at, block:] = jnp.concatenate([tail[: block // 2], tail[block // 2 :]], axis=1).astype(bf16)


def sum_x_kernel(in_ref, out_ref):
    for q in range(in_ref.shape[1]):
        total = in_ref[0, q].astype(f32)
        for p in range(1, in_ref.shape[0]):
            total = total + in_ref[p, q].astype(f32)
        block = out_ref.shape[3]
        rest = EP * CAP - LANES
        tail = jnp.concatenate([total[block:, :rest], total[block:, rest:]], axis=0)
        out_ref[: LANES // CAP, q] = total[:block].T.reshape(LANES // CAP, CAP, block).astype(bf16)
        out_ref[LANES // CAP :, q] = tail.T.reshape(rest // CAP, CAP, block).astype(bf16)

def mix_kernel(got_ref, chosen_ref, out_ref):
    total = got_ref[:, 0].astype(f32)
    for q in range(1, got_ref.shape[1]):
        total = total + got_ref[:, q].astype(f32)
    mixed = jnp.dot(
        chosen_ref[...],
        total.reshape(EP * CAP, out_ref.shape[1]).astype(bf16).astype(f32),
        preferred_element_type=f32,
        precision=lax.Precision.HIGHEST,
    )
    out_ref[...] = mixed.astype(bf16)


def on_device(tokens, norm_gain, route, route_weight, gate_weight, up_weight, down_weight):
    tok_rows, width = tokens.shape
    quarter = width // X
    share = width // TP
    spots = EP * CAP
    ep = ("z", "c")
    inputs = (tokens, norm_gain, route.T, route_weight.T)
    send, chosen = local(
        place_kernel,
        "place",
        [HBM] * 4,
        (pltpu.VMEM((spots, quarter), bf16), pltpu.VMEM((tok_rows, spots), f32)),
        scratch=[pltpu.VMEM(a.shape, a.dtype) for a in inputs]
        + [pltpu.SemaphoreType.DMA((len(inputs),))],
        cost=pl.CostEstimate(flops=10**10, transcendentals=0, bytes_accessed=10**6),
    )(*[far(a) for a in inputs])
    arrived = lax.all_to_all(send.reshape(EP, CAP, quarter), ep, 0, 0, tiled=True)
    rows = lax.all_gather(arrived.reshape(spots, quarter), "x", axis=0, tiled=False)
    count = spots * share // LANES
    quads = Y // 2
    part = local(
        expert_kernel, "expert", [VMEM] * 4, pltpu.VMEM((2 * X, quads, count, LANES), bf16)
    )(near(rows), near(gate_weight[0]), near(up_weight[0]), near(down_weight[0]))
    part = lax.all_to_all(part, ("yp", "x"), 0, 0, tiled=True)
    part = local(sum_x_kernel, "sum_x", [VMEM], pltpu.VMEM((EP, quads, CAP, share), bf16))(
        near(part)
    )
    part = part.reshape(EP * quads, CAP, share)
    part = lax.all_to_all(part, ("z", "c", "yq"), 0, 0, tiled=True)
    back = part.reshape(EP, quads, CAP, share)
    mixed = jax.ShapeDtypeStruct((tok_rows, share), bf16)
    return local(mix_kernel, "mix", [VMEM, VMEM], mixed)(near(back), near(chosen))


def solution(mesh):
    fine = Mesh(mesh.devices.reshape(Z, C, Y // 2, 2, X), ("z", "c", "yq", "yp", "x"))
    ep, tp = ("z", "c"), ("yq", "yp", "x")
    placed = (
        P(ep, None),
        P(),
        P(ep, None),
        P(ep, None),
        P(ep, tp, None),
        P(ep, tp, None),
        P(ep, tp, None),
    )
    return jax.shard_map(
        on_device, mesh=fine, in_specs=placed, out_specs=P(ep, tp), check_vma=False
    )
```

```python
import jax
import jax.numpy as jnp
from jax import lax
from jax.experimental import pallas as pl
from jax.experimental.pallas import tpu as pltpu
from jax.sharding import Mesh
from jax.sharding import PartitionSpec as P

epsilon = 1e-06
bf16 = jnp.bfloat16
f32 = jnp.float32

Z, C, Y, X = 12, 2, 8, 4
EP = Z * C
TP = Y * X
CAP = 8
LANES = 128
SCOPED = 16 << 20
VMEM = pl.BlockSpec(memory_space=pltpu.VMEM)


HBM = pl.BlockSpec(memory_space=pl.ANY)


def near(array):
    return pltpu.with_memory_space_constraint(array, pltpu.VMEM)


def far(array):
    return pltpu.with_memory_space_constraint(array, pltpu.HBM)


def local(kernel, name, specs, outs, scratch=(), cost=None):
    return pl.pallas_call(
        kernel,
        in_specs=specs,
        out_specs=tuple(VMEM for _ in outs) if isinstance(outs, tuple) else VMEM,
        out_shape=outs,
        scratch_shapes=scratch,
        cost_estimate=cost,
        compiler_params=pltpu.CompilerParams(vmem_limit_bytes=SCOPED),
        name=name,
    )


def summed(ref):
    total = ref[0].astype(f32)
    for p in range(1, ref.shape[0]):
        total = total + ref[p].astype(f32)
    return total


def per_slot(table, order):
    rows = table.shape[1]
    lines = [jnp.broadcast_to(table[e : e + 1, :], (CAP, rows)) for e in order]
    return jnp.concatenate(lines, axis=0)


def place_kernel(*refs):
    sources, (send_ref, chosen_ref) = refs[:4], refs[4:6]
    (tokens_ref, gain_ref, route_ref, weight_ref), sems = refs[6:10], refs[10]
    copies = [
        pltpu.make_async_copy(source, there, sems.at[i])
        for i, (source, there) in enumerate(zip(sources, refs[6:10]))
    ]
    for i in (2, 3, 0, 1):
        copies[i].start()
    rows = tokens_ref.shape[0]
    share = send_ref.shape[1]
    before = lax.broadcasted_iota(jnp.int32, (rows, rows), 0) < lax.broadcasted_iota(
        jnp.int32, (rows, rows), 1
    )
    expert = lax.broadcasted_iota(jnp.int32, (EP, rows), 0)
    copies[2].wait()
    copies[3].wait()
    named = jnp.zeros((EP, rows), f32)
    weight = jnp.zeros((EP, rows), f32)
    for k in range(route_ref.shape[0]):
        same = route_ref[k : k + 1, :] == expert
        named = jnp.where(same, 1.0, named)
        weight = jnp.where(same, weight_ref[k : k + 1, :], weight)
    earlier = jnp.dot(named, before.astype(f32), preferred_element_type=f32)
    spot = jnp.where(named > 0.0, earlier, -1.0)
    slot = (lax.broadcasted_iota(jnp.int32, (EP * CAP, rows), 0) % CAP).astype(f32)
    by_core = [z * C + c for c in range(C) for z in range(Z)]
    placing = jnp.where(per_slot(spot, by_core) == slot, 1.0, 0.0).astype(bf16)
    here = per_slot(spot, range(EP)) == slot
    chosen_ref[...] = jnp.where(here, per_slot(weight, range(EP)), 0.0).T
    copies[0].wait()
    copies[1].wait()
    values = tokens_ref[...].astype(f32)
    scale = lax.rsqrt(jnp.mean(values * values, axis=-1, keepdims=True) + epsilon)
    start = pl.multiple_of(lax.axis_index("x") * share, LANES)
    own = tokens_ref[:, pl.ds(start, share)].astype(f32)
    gain = gain_ref[pl.ds(start, share)].reshape(1, share)
    normed = (own * scale * gain).astype(bf16)
    send_ref[...] = jnp.dot(placing, normed, preferred_element_type=f32).astype(bf16)


def expert_kernel(rows_ref, gate_ref, up_ref, down_ref, out_ref):
    parts, _, share = rows_ref.shape
    spans = [slice(p * share, (p + 1) * share) for p in range(parts)]
    contract = (((1,), (1,)), ((), ()))
    gate = up = None
    for p, cols in enumerate(spans):
        g = lax.dot_general(gate_ref[:, cols], rows_ref[p], contract, preferred_element_type=f32)
        gate = g if gate is None else gate + g
    for p, cols in enumerate(spans):
        u = lax.dot_general(up_ref[:, cols], rows_ref[p], contract, preferred_element_type=f32)
        up = u if up is None else up + u
    hidden = (gate / (1.0 + jnp.exp(-gate)) * up).astype(bf16).T
    block = share // Y
    for p, cols in enumerate(spans):
        sums = jnp.dot(hidden, down_ref[:, cols], preferred_element_type=f32).astype(bf16).T
        half = sums.shape[1] // C
        rest = LANES - half
        for c in range(C):
            for i in range(Y):
                piece = sums[i * block : (i + 1) * block, c * half : (c + 1) * half]
                if p < parts - 1:
                    out_ref[c * Y + i, p, :, :half] = piece
                    continue
                for j in range(parts - 1):
                    out_ref[c * Y + i, j, :, half:] = piece[:, j * rest : (j + 1) * rest]


def sum_x_kernel(in_ref, out_ref):
    near_by, lines, block, _ = in_ref.shape
    slots = out_ref.shape[0] * CAP
    for c in range(C):
        total = in_ref[c * Y].astype(f32)
        for i in range(1, near_by // C):
            total = total + in_ref[c * Y + i].astype(f32)
        blocks = [total[q, :, :slots] for q in range(lines)]
        blocks.append(jnp.concatenate([total[q, :, slots:] for q in range(lines)], axis=1))
        for q, piece in enumerate(blocks):
            out_ref[:, q, c] = piece.T.reshape(slots // CAP, CAP, block).astype(bf16)


def mix_kernel(got_ref, chosen_ref, out_ref):
    total = got_ref[:, 0].astype(f32)
    for q in range(1, got_ref.shape[1]):
        total = total + got_ref[:, q].astype(f32)
    mixed = jnp.dot(
        chosen_ref[...],
        total.reshape(EP * CAP, out_ref.shape[1]).astype(bf16).astype(f32),
        preferred_element_type=f32,
        precision=lax.Precision.HIGHEST,
    )
    out_ref[...] = mixed.astype(bf16)


def on_device(tokens, norm_gain, route, route_weight, gate_weight, up_weight, down_weight):
    tok_rows, width = tokens.shape
    quarter = width // X
    share = width // TP
    spots = EP * CAP
    inputs = (tokens, norm_gain, route.T, route_weight.T)
    send, chosen = local(
        place_kernel,
        "place",
        [HBM] * 4,
        (pltpu.VMEM((spots, quarter), bf16), pltpu.VMEM((tok_rows, spots), f32)),
        scratch=[pltpu.VMEM(a.shape, a.dtype) for a in inputs]
        + [pltpu.SemaphoreType.DMA((len(inputs),))],
        cost=pl.CostEstimate(flops=10**10, transcendentals=0, bytes_accessed=10**6),
    )(*[far(a) for a in inputs])
    arrived = lax.all_to_all(send.reshape(EP, CAP, quarter), ("c", "z"), 0, 0, tiled=True)
    rows = lax.all_gather(arrived.reshape(spots, quarter), "x", axis=0, tiled=False)
    quads = Y // 2
    part = local(
        expert_kernel, "expert", [VMEM] * 4, pltpu.VMEM((C * Y, quads - 1, share, LANES), bf16)
    )(near(rows), near(gate_weight[0]), near(up_weight[0]), near(down_weight[0]))
    part = lax.all_to_all(part, ("c", "yp", "x"), 0, 0, tiled=True)
    part = local(sum_x_kernel, "sum_x", [VMEM], pltpu.VMEM((Z, quads, C, CAP, share), bf16))(
        near(part)
    )
    part = part.reshape(Z * quads, C * CAP, share)
    part = lax.all_to_all(part, ("z", "yq"), 0, 0, tiled=True)
    back = part.reshape(Z, quads, C, CAP, share)
    mixed = jax.ShapeDtypeStruct((tok_rows, share), bf16)
    return local(mix_kernel, "mix", [VMEM, VMEM], mixed)(near(back), near(chosen))


def solution(mesh):
    fine = Mesh(mesh.devices.reshape(Z, C, Y // 2, 2, X), ("z", "c", "yq", "yp", "x"))
    ep, tp = ("z", "c"), ("yq", "yp", "x")
    placed = (
        P(ep, None),
        P(),
        P(ep, None),
        P(ep, None),
        P(ep, tp, None),
        P(ep, tp, None),
        P(ep, tp, None),
    )
    return jax.shard_map(
        on_device, mesh=fine, in_specs=placed, out_specs=P(ep, tp), check_vma=False
    )
```

```python
import jax
import jax.numpy as jnp
from jax import lax
from jax.experimental import pallas as pl
from jax.experimental.pallas import tpu as pltpu
from jax.sharding import Mesh
from jax.sharding import PartitionSpec as P

epsilon = 1e-06
bf16 = jnp.bfloat16
f32 = jnp.float32

Z, C, Y, X = 12, 2, 8, 4
EP = Z * C
TP = Y * X
CAP = 8
LANES = 128
SCOPED = 16 << 20
VMEM = pl.BlockSpec(memory_space=pltpu.VMEM)


HBM = pl.BlockSpec(memory_space=pl.ANY)


def near(array):
    return pltpu.with_memory_space_constraint(array, pltpu.VMEM)


def far(array):
    return pltpu.with_memory_space_constraint(array, pltpu.HBM)


def local(kernel, name, specs, outs, scratch=(), cost=None):
    return pl.pallas_call(
        kernel,
        in_specs=specs,
        out_specs=tuple(VMEM for _ in outs) if isinstance(outs, tuple) else VMEM,
        out_shape=outs,
        scratch_shapes=scratch,
        cost_estimate=cost,
        compiler_params=pltpu.CompilerParams(vmem_limit_bytes=SCOPED),
        name=name,
    )


def summed(ref):
    total = ref[0].astype(f32)
    for p in range(1, ref.shape[0]):
        total = total + ref[p].astype(f32)
    return total


def per_slot(table):
    rows = table.shape[1]
    lines = [jnp.broadcast_to(table[e : e + 1, :], (CAP, rows)) for e in range(table.shape[0])]
    return jnp.concatenate(lines, axis=0)


def place_kernel(*refs):
    sources, (send_ref, chosen_ref) = refs[:4], refs[4:6]
    (tokens_ref, gain_ref, route_ref, weight_ref), sems = refs[6:10], refs[10]
    copies = [
        pltpu.make_async_copy(source, there, sems.at[i])
        for i, (source, there) in enumerate(zip(sources, refs[6:10]))
    ]
    for i in (2, 3, 0, 1):
        copies[i].start()
    rows = tokens_ref.shape[0]
    share = send_ref.shape[1]
    before = lax.broadcasted_iota(jnp.int32, (rows, rows), 0) < lax.broadcasted_iota(
        jnp.int32, (rows, rows), 1
    )
    expert = lax.broadcasted_iota(jnp.int32, (EP, rows), 0)
    copies[2].wait()
    copies[3].wait()
    named = jnp.zeros((EP, rows), f32)
    weight = jnp.zeros((EP, rows), f32)
    for k in range(route_ref.shape[0]):
        same = route_ref[k : k + 1, :] == expert
        named = jnp.where(same, 1.0, named)
        weight = jnp.where(same, weight_ref[k : k + 1, :], weight)
    earlier = jnp.dot(
        named.astype(bf16), before.astype(f32).astype(bf16), preferred_element_type=f32
    )
    taken = per_slot(jnp.where(named > 0.0, earlier, -1.0))
    slot = (lax.broadcasted_iota(jnp.int32, taken.shape, 0) % CAP).astype(f32)
    here = taken == slot
    placing = jnp.where(here, 1.0, 0.0).astype(bf16)
    left = jnp.where(here, per_slot(weight), 0.0).T
    for i in range(chosen_ref.shape[0]):
        part = left.astype(bf16)
        chosen_ref[i] = part
        left = left - part.astype(f32)
    copies[0].wait()
    copies[1].wait()
    values = tokens_ref[...].astype(f32)
    scale = lax.rsqrt(jnp.mean(values * values, axis=-1, keepdims=True) + epsilon)
    start = pl.multiple_of(lax.axis_index("x") * share, LANES)
    own = tokens_ref[:, pl.ds(start, share)].astype(f32)
    gain = gain_ref[pl.ds(start, share)].reshape(1, share)
    normed = (own * scale * gain).astype(bf16)
    send_ref[...] = jnp.dot(placing, normed, preferred_element_type=f32).astype(bf16)


def expert_kernel(rows_ref, gate_ref, up_ref, down_ref, out_ref):
    parts, _, share = rows_ref.shape
    spans = [slice(p * share, (p + 1) * share) for p in range(parts)]
    contract = (((1,), (1,)), ((), ()))
    gate = up = None
    for p, cols in enumerate(spans):
        g = lax.dot_general(gate_ref[:, cols], rows_ref[p], contract, preferred_element_type=f32)
        gate = g if gate is None else gate + g
    for p, cols in enumerate(spans):
        u = lax.dot_general(up_ref[:, cols], rows_ref[p], contract, preferred_element_type=f32)
        up = u if up is None else up + u
    hidden = (gate / (1.0 + jnp.exp(-gate)) * up).astype(bf16).T
    block = share // Y
    for p, cols in enumerate(spans):
        sums = jnp.dot(hidden, down_ref[:, cols], preferred_element_type=f32).astype(bf16).T
        for i in range(Y):
            packed(sums[i * block : (i + 1) * block], out_ref.at[i], p)


def packed(piece, out, at):
    block = piece.shape[0]
    tail = piece[:, LANES:]
    out[at, :block] = piece[:, :LANES].astype(bf16)
    out[at, block:] = jnp.concatenate([tail[: block // 2], tail[block // 2 :]], axis=1).astype(bf16)


def sum_x_kernel(in_ref, out_ref):
    for q in range(in_ref.shape[1]):
        total = in_ref[0, q].astype(f32)
        for p in range(1, in_ref.shape[0]):
            total = total + in_ref[p, q].astype(f32)
        total = total.astype(bf16)
        block = out_ref.shape[3]
        rest = EP * CAP - LANES
        tail = jnp.concatenate([total[block:, :rest], total[block:, rest:]], axis=0)
        out_ref[: LANES // CAP, q] = total[:block].T.reshape(LANES // CAP, CAP, block)
        out_ref[LANES // CAP :, q] = tail.T.reshape(rest // CAP, CAP, block)


def mix_kernel(got_ref, chosen_ref, out_ref):
    total = got_ref[:, 0].astype(f32)
    for q in range(1, got_ref.shape[1]):
        total = total + got_ref[:, q].astype(f32)
    rows = total.reshape(EP * CAP, out_ref.shape[1]).astype(bf16)
    mixed = jnp.dot(chosen_ref[0], rows, preferred_element_type=f32)
    for i in range(1, chosen_ref.shape[0]):
        mixed = mixed + jnp.dot(chosen_ref[i], rows, preferred_element_type=f32)
    out_ref[...] = mixed.astype(bf16)


def on_device(tokens, norm_gain, route, route_weight, gate_weight, up_weight, down_weight):
    tok_rows, width = tokens.shape
    quarter = width // X
    share = width // TP
    spots = EP * CAP
    ep = ("z", "c")
    inputs = (tokens, norm_gain, route.T, route_weight.T)
    send, chosen = local(
        place_kernel,
        "place",
        [HBM] * 4,
        (pltpu.VMEM((spots, quarter), bf16), pltpu.VMEM((3, tok_rows, spots), bf16)),
        scratch=[pltpu.VMEM(a.shape, a.dtype) for a in inputs]
        + [pltpu.SemaphoreType.DMA((len(inputs),))],
        cost=pl.CostEstimate(flops=10**10, transcendentals=0, bytes_accessed=10**6),
    )(*[far(a) for a in inputs])
    arrived = lax.all_to_all(send.reshape(EP, CAP, quarter), ep, 0, 0, tiled=True)
    rows = lax.all_gather(arrived.reshape(spots, quarter), "x", axis=0, tiled=False)
    count = spots * share // LANES
    quads = Y // 2
    part = local(
        expert_kernel, "expert", [VMEM] * 4, pltpu.VMEM((2 * X, quads, count, LANES), bf16)
    )(near(rows), near(gate_weight[0]), near(up_weight[0]), near(down_weight[0]))
    part = lax.all_to_all(part, ("yp", "x"), 0, 0, tiled=True)
    part = local(sum_x_kernel, "sum_x", [VMEM], pltpu.VMEM((EP, quads, CAP, share), bf16))(
        near(part)
    )
    part = part.reshape(EP * quads, CAP, share)
    part = lax.all_to_all(part, ("z", "c", "yq"), 0, 0, tiled=True)
    back = part.reshape(EP, quads, CAP, share)
    mixed = jax.ShapeDtypeStruct((tok_rows, share), bf16)
    return local(mix_kernel, "mix", [VMEM, VMEM], mixed)(near(back), near(chosen))


def solution(mesh):
    fine = Mesh(mesh.devices.reshape(Z, C, Y // 2, 2, X), ("z", "c", "yq", "yp", "x"))
    ep, tp = ("z", "c"), ("yq", "yp", "x")
    placed = (
        P(ep, None),
        P(),
        P(ep, None),
        P(ep, None),
        P(ep, tp, None),
        P(ep, tp, None),
        P(ep, tp, None),
    )
    return jax.shard_map(
        on_device, mesh=fine, in_specs=placed, out_specs=P(ep, tp), check_vma=False
    )
```

```python
import jax
import jax.numpy as jnp
from jax import lax
from jax.experimental import pallas as pl
from jax.experimental.pallas import tpu as pltpu
from jax.sharding import Mesh
from jax.sharding import PartitionSpec as P

epsilon = 1e-06
bf16 = jnp.bfloat16
f32 = jnp.float32

Z, C, Y, X = 12, 2, 8, 4
EP = Z * C
TP = Y * X
CAP = 8
LANES = 128
SCOPED = 16 << 20
VMEM = pl.BlockSpec(memory_space=pltpu.VMEM)


HBM = pl.BlockSpec(memory_space=pl.ANY)


def near(array):
    return pltpu.with_memory_space_constraint(array, pltpu.VMEM)


def far(array):
    return pltpu.with_memory_space_constraint(array, pltpu.HBM)


def local(kernel, name, specs, outs, scratch=(), cost=None):
    return pl.pallas_call(
        kernel,
        in_specs=specs,
        out_specs=tuple(VMEM for _ in outs) if isinstance(outs, tuple) else VMEM,
        out_shape=outs,
        scratch_shapes=scratch,
        cost_estimate=cost,
        compiler_params=pltpu.CompilerParams(vmem_limit_bytes=SCOPED),
        name=name,
    )


def summed(ref):
    total = ref[0].astype(f32)
    for p in range(1, ref.shape[0]):
        total = total + ref[p].astype(f32)
    return total


def per_slot(table):
    rows = table.shape[1]
    lines = [jnp.broadcast_to(table[e : e + 1, :], (CAP, rows)) for e in range(table.shape[0])]
    return jnp.concatenate(lines, axis=0)


def spots_of(route_ref):
    rows = route_ref.shape[1]
    expert = lax.broadcasted_iota(jnp.int32, (EP, rows), 0)
    same = [route_ref[k : k + 1, :] == expert for k in range(route_ref.shape[0])]
    named = jnp.zeros((EP, rows), f32)
    for hit in same:
        named = jnp.where(hit, 1.0, named)
    before = lax.broadcasted_iota(jnp.int32, (rows, rows), 0) < lax.broadcasted_iota(
        jnp.int32, (rows, rows), 1
    )
    earlier = jnp.dot(
        named.astype(bf16), before.astype(f32).astype(bf16), preferred_element_type=f32
    )
    taken = per_slot(jnp.where(named > 0.0, earlier, -1.0))
    slot = (lax.broadcasted_iota(jnp.int32, taken.shape, 0) % CAP).astype(f32)
    return same, taken == slot


def place_kernel(*refs):
    sources, send_ref = refs[:3], refs[3]
    (tokens_ref, gain_ref, route_ref), sems = refs[4:7], refs[7]
    copies = [
        pltpu.make_async_copy(source, there, sems.at[i])
        for i, (source, there) in enumerate(zip(sources, refs[4:7]))
    ]
    for i in (2, 0, 1):
        copies[i].start()
    share = send_ref.shape[1]
    copies[2].wait()
    _, here = spots_of(route_ref)
    placing = jnp.where(here, 1.0, 0.0).astype(bf16)
    copies[0].wait()
    copies[1].wait()
    values = tokens_ref[...].astype(f32)
    scale = lax.rsqrt(jnp.mean(values * values, axis=-1, keepdims=True) + epsilon)
    start = pl.multiple_of(lax.axis_index("x") * share, LANES)
    own = tokens_ref[:, pl.ds(start, share)].astype(f32)
    gain = gain_ref[pl.ds(start, share)].reshape(1, share)
    normed = (own * scale * gain).astype(bf16)
    send_ref[...] = jnp.dot(placing, normed, preferred_element_type=f32).astype(bf16)


def weigh_kernel(route_ref, weight_ref, chosen_ref):
    same, here = spots_of(route_ref)
    weight = jnp.zeros((EP, route_ref.shape[1]), f32)
    for k, hit in enumerate(same):
        weight = jnp.where(hit, weight_ref[k : k + 1, :], weight)
    left = jnp.where(here, per_slot(weight), 0.0).T
    for i in range(chosen_ref.shape[0]):
        part = left.astype(bf16)
        chosen_ref[i] = part
        left = left - part.astype(f32)


def expert_kernel(rows_ref, gate_ref, up_ref, down_ref, out_ref):
    parts, _, share = rows_ref.shape
    spans = [slice(p * share, (p + 1) * share) for p in range(parts)]
    contract = (((1,), (1,)), ((), ()))
    gate = up = None
    for p, cols in enumerate(spans):
        g = lax.dot_general(gate_ref[:, cols], rows_ref[p], contract, preferred_element_type=f32)
        gate = g if gate is None else gate + g
    for p, cols in enumerate(spans):
        u = lax.dot_general(up_ref[:, cols], rows_ref[p], contract, preferred_element_type=f32)
        up = u if up is None else up + u
    hidden = (gate / (1.0 + jnp.exp(-gate)) * up).astype(bf16).T
    block = share // Y
    for p, cols in enumerate(spans):
        sums = jnp.dot(hidden, down_ref[:, cols], preferred_element_type=f32).astype(bf16).T
        for i in range(Y):
            packed(sums[i * block : (i + 1) * block], out_ref.at[i], p)


def packed(piece, out, at):
    block = piece.shape[0]
    tail = piece[:, LANES:]
    out[at, :block] = piece[:, :LANES].astype(bf16)
    out[at, block:] = jnp.concatenate([tail[: block // 2], tail[block // 2 :]], axis=1).astype(bf16)


def sum_x_kernel(in_ref, out_ref):
    for q in range(in_ref.shape[1]):
        total = in_ref[0, q].astype(f32)
        for p in range(1, in_ref.shape[0]):
            total = total + in_ref[p, q].astype(f32)
        total = total.astype(bf16)
        block = out_ref.shape[3]
        rest = EP * CAP - LANES
        tail = jnp.concatenate([total[block:, :rest], total[block:, rest:]], axis=0)
        out_ref[: LANES // CAP, q] = total[:block].T.reshape(LANES // CAP, CAP, block)
        out_ref[LANES // CAP :, q] = tail.T.reshape(rest // CAP, CAP, block)


def mix_kernel(got_ref, chosen_ref, out_ref):
    total = got_ref[:, 0].astype(f32)
    for q in range(1, got_ref.shape[1]):
        total = total + got_ref[:, q].astype(f32)
    rows = total.reshape(EP * CAP, out_ref.shape[1]).astype(bf16)
    mixed = jnp.dot(chosen_ref[0], rows, preferred_element_type=f32)
    for i in range(1, chosen_ref.shape[0]):
        mixed = mixed + jnp.dot(chosen_ref[i], rows, preferred_element_type=f32)
    out_ref[...] = mixed.astype(bf16)


def on_device(tokens, norm_gain, route, route_weight, gate_weight, up_weight, down_weight):
    tok_rows, width = tokens.shape
    quarter = width // X
    share = width // TP
    spots = EP * CAP
    ep = ("z", "c")
    inputs = (tokens, norm_gain, route.T)
    send = local(
        place_kernel,
        "place",
        [HBM] * 3,
        pltpu.VMEM((spots, quarter), bf16),
        scratch=[pltpu.VMEM(a.shape, a.dtype) for a in inputs]
        + [pltpu.SemaphoreType.DMA((len(inputs),))],
        cost=pl.CostEstimate(flops=10**10, transcendentals=0, bytes_accessed=10**6),
    )(*[far(a) for a in inputs])
    chosen = local(
        weigh_kernel,
        "weigh",
        [VMEM] * 2,
        pltpu.VMEM((3, tok_rows, spots), bf16),
        cost=pl.CostEstimate(flops=10**9, transcendentals=0, bytes_accessed=10**5),
    )(near(route.T), near(route_weight.T))
    arrived = lax.all_to_all(send.reshape(EP, CAP, quarter), ep, 0, 0, tiled=True)
    rows = lax.all_gather(arrived.reshape(spots, quarter), "x", axis=0, tiled=False)
    count = spots * share // LANES
    quads = Y // 2
    part = local(
        expert_kernel, "expert", [VMEM] * 4, pltpu.VMEM((2 * X, quads, count, LANES), bf16)
    )(near(rows), near(gate_weight[0]), near(up_weight[0]), near(down_weight[0]))
    part = lax.all_to_all(part, ("yp", "x"), 0, 0, tiled=True)
    part = local(sum_x_kernel, "sum_x", [VMEM], pltpu.VMEM((EP, quads, CAP, share), bf16))(
        near(part)
    )
    part = part.reshape(EP * quads, CAP, share)
    part = lax.all_to_all(part, ("z", "c", "yq"), 0, 0, tiled=True)
    back = part.reshape(EP, quads, CAP, share)
    mixed = jax.ShapeDtypeStruct((tok_rows, share), bf16)
    return local(mix_kernel, "mix", [VMEM, VMEM], mixed)(near(back), near(chosen))


def solution(mesh):
    fine = Mesh(mesh.devices.reshape(Z, C, Y // 2, 2, X), ("z", "c", "yq", "yp", "x"))
    ep, tp = ("z", "c"), ("yq", "yp", "x")
    placed = (
        P(ep, None),
        P(),
        P(ep, None),
        P(ep, None),
        P(ep, tp, None),
        P(ep, tp, None),
        P(ep, tp, None),
    )
    return jax.shard_map(
        on_device, mesh=fine, in_specs=placed, out_specs=P(ep, tp), check_vma=False
    )
```

```python
import jax
import jax.numpy as jnp
from jax import lax
from jax.experimental import pallas as pl
from jax.experimental.pallas import tpu as pltpu
from jax.sharding import Mesh
from jax.sharding import PartitionSpec as P

epsilon = 1e-06
bf16 = jnp.bfloat16
f32 = jnp.float32

Z, C, Y, X = 12, 2, 8, 4
EP = Z * C
TP = Y * X
CAP = 8
LANES = 128
SCOPED = 16 << 20
VMEM = pl.BlockSpec(memory_space=pltpu.VMEM)


HBM = pl.BlockSpec(memory_space=pl.ANY)


def near(array):
    return pltpu.with_memory_space_constraint(array, pltpu.VMEM)


def far(array):
    return pltpu.with_memory_space_constraint(array, pltpu.HBM)


def local(kernel, name, specs, outs, scratch=(), cost=None):
    return pl.pallas_call(
        kernel,
        in_specs=specs,
        out_specs=tuple(VMEM for _ in outs) if isinstance(outs, tuple) else VMEM,
        out_shape=outs,
        scratch_shapes=scratch,
        cost_estimate=cost,
        compiler_params=pltpu.CompilerParams(vmem_limit_bytes=SCOPED),
        name=name,
    )


def summed(ref):
    total = ref[0].astype(f32)
    for p in range(1, ref.shape[0]):
        total = total + ref[p].astype(f32)
    return total


def per_slot(table):
    rows = table.shape[1]
    lines = [jnp.broadcast_to(table[e : e + 1, :], (CAP, rows)) for e in range(table.shape[0])]
    return jnp.concatenate(lines, axis=0)


def place_kernel(*refs):
    sources, (send_ref, chosen_ref) = refs[:4], refs[4:6]
    (tokens_ref, gain_ref, route_ref, weight_ref), sems = refs[6:10], refs[10]
    copies = [
        pltpu.make_async_copy(source, there, sems.at[i])
        for i, (source, there) in enumerate(zip(sources, refs[6:10]))
    ]
    for i in (0, 2, 3, 1):
        copies[i].start()
    rows = tokens_ref.shape[0]
    share = send_ref.shape[1]
    before = lax.broadcasted_iota(jnp.int32, (rows, rows), 0) < lax.broadcasted_iota(
        jnp.int32, (rows, rows), 1
    )
    expert = lax.broadcasted_iota(jnp.int32, (EP, rows), 0)
    copies[2].wait()
    copies[3].wait()
    named = jnp.zeros((EP, rows), f32)
    weight = jnp.zeros((EP, rows), f32)
    for k in range(route_ref.shape[0]):
        same = route_ref[k : k + 1, :] == expert
        named = jnp.where(same, 1.0, named)
        weight = jnp.where(same, weight_ref[k : k + 1, :], weight)
    earlier = jnp.dot(
        named.astype(bf16), before.astype(f32).astype(bf16), preferred_element_type=f32
    )
    taken = per_slot(jnp.where(named > 0.0, earlier, -1.0))
    slot = (lax.broadcasted_iota(jnp.int32, taken.shape, 0) % CAP).astype(f32)
    here = taken == slot
    placing = jnp.where(here, 1.0, 0.0).astype(bf16)
    left = jnp.where(here, per_slot(weight), 0.0).T
    for i in range(chosen_ref.shape[0]):
        part = left.astype(bf16)
        chosen_ref[i] = part
        left = left - part.astype(f32)
    copies[0].wait()
    copies[1].wait()
    values = tokens_ref[...].astype(f32)
    scale = lax.rsqrt(jnp.mean(values * values, axis=-1, keepdims=True) + epsilon)
    start = pl.multiple_of(lax.axis_index("x") * share, LANES)
    own = tokens_ref[:, pl.ds(start, share)].astype(f32)
    gain = gain_ref[pl.ds(start, share)].reshape(1, share)
    normed = (own * scale * gain).astype(bf16)
    send_ref[...] = jnp.dot(placing, normed, preferred_element_type=f32).astype(bf16)


def expert_kernel(rows_ref, gate_ref, up_ref, down_ref, out_ref):
    parts, _, share = rows_ref.shape
    spans = [slice(p * share, (p + 1) * share) for p in range(parts)]
    contract = (((1,), (1,)), ((), ()))
    gate = up = None
    for p, cols in enumerate(spans):
        g = lax.dot_general(gate_ref[:, cols], rows_ref[p], contract, preferred_element_type=f32)
        gate = g if gate is None else gate + g
    for p, cols in enumerate(spans):
        u = lax.dot_general(up_ref[:, cols], rows_ref[p], contract, preferred_element_type=f32)
        up = u if up is None else up + u
    hidden = (gate / (1.0 + jnp.exp(-gate)) * up).astype(bf16).T
    block = share // Y
    for p, cols in enumerate(spans):
        sums = jnp.dot(hidden, down_ref[:, cols], preferred_element_type=f32).astype(bf16).T
        for i in range(Y):
            packed(sums[i * block : (i + 1) * block], out_ref.at[i], p)


def packed(piece, out, at):
    block = piece.shape[0]
    tail = piece[:, LANES:]
    out[at, :block] = piece[:, :LANES].astype(bf16)
    out[at, block:] = jnp.concatenate([tail[: block // 2], tail[block // 2 :]], axis=1).astype(bf16)


def sum_x_kernel(in_ref, out_ref):
    for q in range(in_ref.shape[1]):
        total = in_ref[0, q].astype(f32)
        for p in range(1, in_ref.shape[0]):
            total = total + in_ref[p, q].astype(f32)
        total = total.astype(bf16)
        block = out_ref.shape[3]
        rest = EP * CAP - LANES
        tail = jnp.concatenate([total[block:, :rest], total[block:, rest:]], axis=0)
        out_ref[: LANES // CAP, q] = total[:block].T.reshape(LANES // CAP, CAP, block)
        out_ref[LANES // CAP :, q] = tail.T.reshape(rest // CAP, CAP, block)


def mix_kernel(got_ref, chosen_ref, out_ref):
    total = got_ref[:, 0].astype(f32)
    for q in range(1, got_ref.shape[1]):
        total = total + got_ref[:, q].astype(f32)
    rows = total.reshape(EP * CAP, out_ref.shape[1]).astype(bf16)
    mixed = jnp.dot(chosen_ref[0], rows, preferred_element_type=f32)
    for i in range(1, chosen_ref.shape[0]):
        mixed = mixed + jnp.dot(chosen_ref[i], rows, preferred_element_type=f32)
    out_ref[...] = mixed.astype(bf16)


def on_device(tokens, norm_gain, route, route_weight, gate_weight, up_weight, down_weight):
    tok_rows, width = tokens.shape
    quarter = width // X
    share = width // TP
    spots = EP * CAP
    ep = ("z", "c")
    inputs = (tokens, norm_gain, route.T, route_weight.T)
    send, chosen = local(
        place_kernel,
        "place",
        [HBM] * 4,
        (pltpu.VMEM((spots, quarter), bf16), pltpu.VMEM((3, tok_rows, spots), bf16)),
        scratch=[pltpu.VMEM(a.shape, a.dtype) for a in inputs]
        + [pltpu.SemaphoreType.DMA((len(inputs),))],
        cost=pl.CostEstimate(flops=10**10, transcendentals=0, bytes_accessed=10**6),
    )(*[far(a) for a in inputs])
    arrived = lax.all_to_all(send.reshape(EP, CAP, quarter), ep, 0, 0, tiled=True)
    rows = lax.all_gather(arrived.reshape(spots, quarter), "x", axis=0, tiled=False)
    count = spots * share // LANES
    quads = Y // 2
    part = local(
        expert_kernel, "expert", [VMEM] * 4, pltpu.VMEM((2 * X, quads, count, LANES), bf16)
    )(near(rows), near(gate_weight[0]), near(up_weight[0]), near(down_weight[0]))
    part = lax.all_to_all(part, ("yp", "x"), 0, 0, tiled=True)
    part = local(sum_x_kernel, "sum_x", [VMEM], pltpu.VMEM((EP, quads, CAP, share), bf16))(
        near(part)
    )
    part = part.reshape(EP * quads, CAP, share)
    part = lax.all_to_all(part, ("z", "c", "yq"), 0, 0, tiled=True)
    back = part.reshape(EP, quads, CAP, share)
    mixed = jax.ShapeDtypeStruct((tok_rows, share), bf16)
    return local(mix_kernel, "mix", [VMEM, VMEM], mixed)(near(back), near(chosen))


def solution(mesh):
    fine = Mesh(mesh.devices.reshape(Z, C, Y // 2, 2, X), ("z", "c", "yq", "yp", "x"))
    ep, tp = ("z", "c"), ("yq", "yp", "x")
    placed = (
        P(ep, None),
        P(),
        P(ep, None),
        P(ep, None),
        P(ep, tp, None),
        P(ep, tp, None),
        P(ep, tp, None),
    )
    return jax.shard_map(
        on_device, mesh=fine, in_specs=placed, out_specs=P(ep, tp), check_vma=False
    )
```
